32 devices in a mesh: rep: 2 (over x), fs: 8 (over z, y), tp: 2 (over core).
Axes of the slice: x: 2, y: 2, z: 4, core: 2. Of those that a mesh axis runs over, the one named last changes fastest.
Arguments:
- tokens: bfloat16 [16, 512, 2048], P(('rep', 'fs')), may hold values from -6 to 6
- gain_mix_pre: float32 [2048], P('fs'), may hold values from 0.1 to 1.9
- gain_mix_post: float32 [2048], P('fs'), may hold values from 0.1 to 1.9
- gain_mlp_pre: float32 [2048], P('fs'), may hold values from 0.1 to 1.9
- gain_mlp_post: float32 [2048], P('fs'), may hold values from 0.1 to 1.9
- x_weight: float32 [2048, 2048], P('fs', 'tp'), may hold values from -0.125 to 0.125
- gate_weight: float32 [2048, 2048], P('fs', 'tp'), may hold values from -0.125 to 0.125
- x_scale: float32 [2048], P('tp'), may hold values from 0.5 to 2
- gate_scale: float32 [2048], P('tp'), may hold values from 0.5 to 2
- conv_weight: float32 [4, 2048], P(None, 'tp'), may hold values from -3 to 3
- recur_map: bfloat16 [2048, 32], P('tp'), may hold values from -1 to 1
- input_map: bfloat16 [2048, 32], P('tp'), may hold values from -1 to 1
- decay_param: float32 [2048], P('tp'), may hold values from 3.9 to 10
- out_weight: float32 [2048, 2048], P('tp', 'fs'), may hold values from -0.125 to 0.125
- out_scale: float32 [2048], P('fs'), may hold values from 0.5 to 2
- up_weight: float32 [2048, 6144], P('fs', 'tp'), may hold values from -0.125 to 0.125
- up_scale: float32 [6144], P('tp'), may hold values from 0.5 to 2
- down_weight: float32 [6144, 2048], P('tp', 'fs'), may hold values from -0.078125 to 0.078125
- down_scale: float32 [2048], P('fs'), may hold values from 0.5 to 2
Outputs:
- layer_out: bfloat16 [16, 512, 2048], P(('rep', 'fs'), 'tp')
The draws below stay inside these ranges and needn't reach their ends.
All inputs are finite; a program needn't handle non-finite values.
Results may differ from the reference program's by a relative error of at most 0.025.
Values may be sent and summed in bfloat16 or wider, within the bound.
A program may use at most 128 MiB of HBM per device.

```python
import math
import jax
import jax.numpy as jnp
from jax import lax

D = 2048
W = 2048
FF = 6144
BLOCK = 32
CONV = 4
SEQ = 512
SEQS = 16
N_TP = 2


def draw_decay_param(key, part):
    keys = jax.random.split(jax.random.fold_in(key, 11), 2)
    slow_share = 0.5
    chooser = jax.random.uniform(keys[0], (W,), jnp.float32)
    spread = jax.random.uniform(keys[1], (W,), jnp.float32)
    slow_rate = jnp.minimum(jnp.exp(jnp.log(0.05 / SEQ) + spread * jnp.log(10.0)), 0.02)
    fast_rate = jnp.exp(jnp.log(0.004) + spread * jnp.log(5.0))
    rate = jnp.where(chooser < slow_share, slow_rate, fast_rate)
    return (-jnp.log(jnp.expm1(rate))).astype(jnp.float32)


def block_scale(key, shape, shards, low, largest):
    gain, own = 1.0, jax.random.fold_in(key, 6)
    for axis_at, blocks in shards:
        draws = jnp.exp(jax.random.uniform(jax.random.fold_in(own, axis_at), (blocks,), jnp.float32, low / len(shards), largest / len(shards)))
        gain = gain * jnp.repeat(draws, shape[axis_at] // blocks).reshape([-1 if axis == axis_at else 1 for axis in range(len(shape))])
    return gain


def normal_values(stream_key, shape, deviation, bound, cuts=(), dtype=jnp.bfloat16):
    level = block_scale(stream_key, shape, cuts, -0.22, 0.18) if cuts else 1.0
    result = jax.random.normal(stream_key, shape, jnp.float32) * deviation * level
    return jnp.minimum(jnp.maximum(result, -bound), bound).astype(dtype)


def setup_inputs(seed: int = 0) -> dict:
    streams_of = jax.random.split(jax.random.key(seed), 20)
    tokens = normal_values(streams_of[0], (SEQS, SEQ, D), 1.0, 6.0, ((0, 16),))
    gain_mix_pre = jnp.clip(1.0 + 0.18 * jax.random.normal(streams_of[1], (D,), jnp.float32), 0.1, 1.9)
    gain_mix_post = jnp.clip(1.0 + 0.18 * jax.random.normal(streams_of[2], (D,), jnp.float32), 0.1, 1.9)
    gain_mlp_pre = jnp.clip(1.0 + 0.18 * jax.random.normal(streams_of[3], (D,), jnp.float32), 0.1, 1.9)
    gain_mlp_post = jnp.clip(1.0 + 0.18 * jax.random.normal(streams_of[4], (D,), jnp.float32), 0.1, 1.9)
    x_weight = normal_values(streams_of[5], (D, W), D ** -0.5, 0.125, ((0, 8), (1, 2)), jnp.float32)
    gate_weight = normal_values(streams_of[6], (D, W), D ** -0.5, 0.125, ((0, 8), (1, 2)), jnp.float32)
    x_scale = jnp.clip(jnp.exp(math.log(2.0) - 1.3862944 * jax.random.uniform(streams_of[7], (W,), jnp.float32) ** block_scale(streams_of[7], (W,), ((0, 2),), -0.2, 0.2)), 0.5, 2.0)
    gate_scale = jnp.clip(jnp.exp(math.log(2.0) - 1.3862944 * jax.random.uniform(streams_of[8], (W,), jnp.float32) ** block_scale(streams_of[8], (W,), ((0, 2),), -0.2, 0.2)), 0.5, 2.0)
    conv_weight = normal_values(streams_of[9], (CONV, W), 0.5, 3.0, ((1, 2),), jnp.float32)
    recur_map = normal_values(streams_of[10], (W, BLOCK), BLOCK ** -0.5, 1.0, ((0, 2),))
    input_map = normal_values(streams_of[11], (W, BLOCK), BLOCK ** -0.5, 1.0, ((0, 2),))
    decay_param = draw_decay_param(jax.random.fold_in(streams_of[19], 71), 0)
    out_weight = normal_values(streams_of[13], (W, D), W ** -0.5, 0.125, ((0, 2), (1, 8)), jnp.float32)
    out_scale = jnp.clip(jnp.exp(math.log(2.0) - 1.3862944 * jax.random.uniform(streams_of[14], (D,), jnp.float32) ** block_scale(streams_of[14], (D,), ((0, 8),), -0.2, 0.2)), 0.5, 2.0)
    up_weight = normal_values(streams_of[15], (D, FF), D ** -0.5, 0.125, ((0, 8), (1, 2)), jnp.float32)
    up_scale = jnp.clip(jnp.exp(math.log(2.0) - 1.3862944 * jax.random.uniform(streams_of[16], (FF,), jnp.float32) ** block_scale(streams_of[16], (FF,), ((0, 2),), -0.2, 0.2)), 0.5, 2.0)
    down_weight = normal_values(streams_of[17], (FF, D), FF ** -0.5, 0.078125, ((0, 2), (1, 8)), jnp.float32)
    down_scale = jnp.clip(jnp.exp(math.log(2.0) - 1.3862944 * jax.random.uniform(streams_of[18], (D,), jnp.float32) ** block_scale(streams_of[18], (D,), ((0, 8),), -0.2, 0.2)), 0.5, 2.0)
    return dict(tokens=tokens, gain_mix_pre=gain_mix_pre, gain_mix_post=gain_mix_post, gain_mlp_pre=gain_mlp_pre, gain_mlp_post=gain_mlp_post, x_weight=x_weight, gate_weight=gate_weight, x_scale=x_scale, gate_scale=gate_scale, conv_weight=conv_weight, recur_map=recur_map, input_map=input_map, decay_param=decay_param, out_weight=out_weight, out_scale=out_scale, up_weight=up_weight, up_scale=up_scale, down_weight=down_weight, down_scale=down_scale)


EPSILON = 1e-06
DECAY_SCALE = 8.0

def rms_rows(values, gain_vector):
    return values * lax.rsqrt(lax.optimization_barrier(jnp.mean(values * values, axis=-1, keepdims=True)) + EPSILON) * gain_vector

def link_states(earlier, later):
    return (earlier[0] * later[0], later[0] * earlier[1] + later[1])

def reference(tokens, gain_mix_pre, gain_mix_post, gain_mlp_pre, gain_mlp_post, x_weight, gate_weight, x_scale, gate_scale, conv_weight, recur_map, input_map, decay_param, out_weight, out_scale, up_weight, up_scale, down_weight, down_scale):
    x_bf = x_weight.astype(jnp.bfloat16)
    gate_bf = gate_weight.astype(jnp.bfloat16)
    out_bf = out_weight.astype(jnp.bfloat16)
    up_bf = up_weight.astype(jnp.bfloat16)
    down_bf = down_weight.astype(jnp.bfloat16)
    blocks = W // BLOCK
    recur_blocks = recur_map.astype(jnp.float32).reshape(blocks, BLOCK, BLOCK)
    input_blocks = input_map.astype(jnp.float32).reshape(blocks, BLOCK, BLOCK)
    hidden_group = FF // N_TP
    channel_group = W // N_TP

    def one_sequence(seq_tokens):
        resid_in = seq_tokens.astype(jnp.float32)
        normed = rms_rows(resid_in, gain_mix_pre).astype(jnp.bfloat16)
        x_branch = (jnp.dot(normed, x_bf, preferred_element_type=jnp.float32) * x_scale).astype(jnp.bfloat16)
        gate_branch = (jnp.dot(normed, gate_bf, preferred_element_type=jnp.float32) * gate_scale).astype(jnp.bfloat16)
        padded = jnp.concatenate([jnp.zeros((CONV - 1, W), jnp.bfloat16), x_branch], axis=0)
        conv_sum = jnp.zeros((SEQ, W), jnp.float32)
        for tap_index in range(CONV):
            conv_sum = conv_sum + conv_weight[tap_index] * padded[tap_index:tap_index + SEQ].astype(jnp.float32)
        conv_out = lax.optimization_barrier(conv_sum.astype(jnp.bfloat16)).astype(jnp.float32)
        conv_blocks = conv_out.reshape(SEQ, blocks, BLOCK)
        recur_logit = jnp.einsum('tnc,ncd->tnd', conv_blocks, recur_blocks, precision=lax.Precision.HIGHEST).reshape(SEQ, W)
        input_logit = jnp.einsum('tnc,ncd->tnd', conv_blocks, input_blocks, precision=lax.Precision.HIGHEST).reshape(SEQ, W)
        log_decay = -DECAY_SCALE * jax.nn.sigmoid(recur_logit) * jax.nn.softplus(-decay_param)
        drive = jnp.sqrt(-jnp.expm1(2.0 * log_decay)) * jax.nn.sigmoid(input_logit) * conv_out
        _, states = lax.associative_scan(link_states, (jnp.exp(log_decay), drive), axis=0)
        mixed = (states * jax.nn.gelu(gate_branch.astype(jnp.float32))).astype(jnp.bfloat16)
        mix_sum = jnp.zeros((SEQ, D), jnp.float32)
        for group_index in range(N_TP):
            first_col = group_index * channel_group
            mix_part = jnp.dot(mixed[:, first_col:first_col + channel_group], out_bf[first_col:first_col + channel_group], preferred_element_type=jnp.float32) * out_scale
            mix_sum = mix_sum + lax.optimization_barrier(mix_part.astype(jnp.bfloat16)).astype(jnp.float32)
        hidden_state = (resid_in + rms_rows(mix_sum, gain_mix_post)).astype(jnp.bfloat16)
        normed_mlp = rms_rows(hidden_state.astype(jnp.float32), gain_mlp_pre).astype(jnp.bfloat16)
        up_proj = jnp.dot(normed_mlp, up_bf, preferred_element_type=jnp.float32) * up_scale
        activated = jnp.square(jax.nn.relu(up_proj)).astype(jnp.bfloat16)
        mlp_sum = jnp.zeros((SEQ, D), jnp.float32)
        for group_index in range(N_TP):
            first_col = group_index * hidden_group
            partial_value = jnp.dot(activated[:, first_col:first_col + hidden_group], down_bf[first_col:first_col + hidden_group], preferred_element_type=jnp.float32) * down_scale
            mlp_sum = mlp_sum + lax.optimization_barrier(partial_value.astype(jnp.bfloat16)).astype(jnp.float32)
        return (hidden_state.astype(jnp.float32) + rms_rows(mlp_sum, gain_mlp_post)).astype(jnp.bfloat16)
    return lax.map(one_sequence, tokens)
```

```python
import functools

import jax
import jax.numpy as jnp
from jax import lax
from jax.experimental import pallas as pl
from jax.experimental.pallas import tpu as pltpu
from jax.sharding import PartitionSpec as P

BLOCK = 32
LANES = 128
EPSILON = 1e-06
DECAY_SCALE = 8.0
F32 = jnp.float32
BF16 = jnp.bfloat16


def unit_rows(values):
    return values * lax.rsqrt(jnp.mean(values * values, axis=-1, keepdims=True) + EPSILON)


def shifted(values, distance, fill):
    head = jnp.full((distance, values.shape[1]), fill, values.dtype)
    return jnp.concatenate([head, values[: values.shape[0] - distance]], axis=0)


def mixer_kernel(x_ref, gate_ref, taps_ref, recur_ref, input_ref, rate_ref, mixed_ref):
    length = x_ref.shape[0]
    x_branch = x_ref[...].astype(F32)
    taps = taps_ref.shape[0]
    total = taps_ref[taps - 1 : taps, :] * x_branch
    for tap in range(taps - 1):
        total += taps_ref[tap : tap + 1, :] * shifted(x_branch, taps - 1 - tap, 0.0)
    conv = total.astype(BF16)
    recur = jax.nn.sigmoid(jnp.dot(conv, recur_ref[...], preferred_element_type=F32))
    gate_in = jax.nn.sigmoid(jnp.dot(conv, input_ref[...], preferred_element_type=F32))
    log_decay = recur * rate_ref[0:1, :]
    decay = jnp.exp(log_decay)
    z = -2.0 * log_decay
    series = z * (1.0 - z * (1 / 2) * (1.0 - z * (1 / 3) * (1.0 - z * (1 / 4) * (1.0 - z * (1 / 5)))))
    power = jnp.where(z < 0.1, series, 1.0 - decay * decay)
    state = jnp.sqrt(power) * gate_in * conv.astype(F32)
    distance = 1
    while distance < length:
        state = state + decay * shifted(state, distance, 0.0)
        decay = decay * shifted(decay, distance, 1.0)
        distance *= 2
    mixed_ref[...] = (state * jax.nn.gelu(gate_ref[...].astype(F32))).astype(BF16)


def mixer(branches, taps, recur_dense, input_dense, rate, sequences):
    rows, width = branches.shape[0], branches.shape[1] // 2
    length = rows // sequences
    groups = width // LANES
    return pl.pallas_call(
        mixer_kernel,
        grid=(sequences, groups),
        in_specs=[
            pl.BlockSpec((length, LANES), lambda s, g: (s, g)),
            pl.BlockSpec((length, LANES), lambda s, g: (s, g + groups)),
            pl.BlockSpec((taps.shape[0], LANES), lambda s, g: (0, g)),
            pl.BlockSpec((LANES, LANES), lambda s, g: (g, 0)),
            pl.BlockSpec((LANES, LANES), lambda s, g: (g, 0)),
            pl.BlockSpec((1, LANES), lambda s, g: (0, g)),
        ],
        out_specs=pl.BlockSpec((length, LANES), lambda s, g: (s, g)),
        out_shape=jax.ShapeDtypeStruct((rows, width), BF16),
        cost_estimate=pl.CostEstimate(
            flops=rows * width * 100, bytes_accessed=rows * width * 6, transcendentals=rows * width * 4
        ),
        name="mixer",
    )(branches, branches, taps, recur_dense, input_dense, rate)


def on_device(
    tokens, gain_mix_pre, gain_mix_post, gain_mlp_pre, gain_mlp_post,
    x_weight, gate_weight, x_scale, gate_scale, conv_weight, recur_map, input_map,
    decay_param, out_weight, out_scale, up_weight, up_scale, down_weight, down_scale,
):
    reps = lax.axis_size("rep")
    rep = lax.axis_index("rep")
    team = ("rep", "tp")

    def part(values, axis):
        size = values.shape[axis] // reps
        return lax.dynamic_slice_in_dim(values, rep * size, size, axis)

    length = tokens.shape[1]
    share_rows = length // lax.axis_size("tp")
    offset_row = lax.axis_index("tp") * share_rows
    resid_share = lax.dynamic_slice_in_dim(tokens[0], offset_row, share_rows, 0).astype(F32)
    normed = lax.all_gather(unit_rows(resid_share).astype(BF16), team, axis=0, tiled=True)

    pre = gain_mix_pre[:, None]
    branch_rows = jnp.concatenate(
        [(part(x_weight, 1) * pre).astype(BF16), (part(gate_weight, 1) * pre).astype(BF16)], axis=1
    )
    branch_full = lax.all_gather(branch_rows, "fs", axis=0, tiled=True)
    post = jnp.stack([gain_mix_post, gain_mlp_post])
    post_high = post.astype(BF16)
    post_low = (post - post_high.astype(F32)).astype(BF16)
    pad_rows = jnp.zeros((12, post.shape[1]), BF16)
    out_cols = jnp.concatenate(
        [(part(out_weight, 0) * out_scale).astype(BF16), post_high, post_low, pad_rows], axis=0
    )
    out_all = lax.all_gather(out_cols, "fs", axis=1, tiled=True)
    up_full = lax.all_gather(
        (part(up_weight, 1) * gain_mlp_pre[:, None]).astype(BF16), "fs", axis=0, tiled=True
    )
    down_full = lax.all_gather((part(down_weight, 0) * down_scale).astype(BF16), "fs", axis=1, tiled=True)

    scales = jnp.concatenate([part(x_scale, 0), part(gate_scale, 0)])
    branches = (jnp.dot(normed, branch_full, preferred_element_type=F32) * scales).astype(BF16)
    width = branches.shape[1] // 2

    def dense(block_map):
        rows = lax.broadcasted_iota(jnp.int32, (width, LANES), 0)
        columns = lax.broadcasted_iota(jnp.int32, (width, LANES), 1)
        spread = jnp.tile(part(block_map, 0), (1, LANES // BLOCK))
        return jnp.where(rows % LANES // BLOCK == columns // BLOCK, spread, 0).astype(BF16)

    rate = -DECAY_SCALE * jax.nn.softplus(-part(decay_param, 0))
    mixed = mixer(
        branches, part(conv_weight, 1), dense(recur_map), dense(input_map), rate[None], reps
    )
    out_full = out_all[:width]
    gains = out_all[width : width + 2].astype(F32) + out_all[width + 2 : width + 4].astype(F32)
    mix_share = lax.psum_scatter(
        jnp.dot(mixed, out_full, preferred_element_type=F32).astype(BF16),
        team, scatter_dimension=0, tiled=True,
    ).astype(F32)
    hidden_state = (resid_share + unit_rows(mix_share) * gains[0]).astype(BF16)
    mlp_input = lax.all_gather(
        unit_rows(hidden_state.astype(F32)).astype(BF16), team, axis=0, tiled=True
    )
    up_proj = jnp.dot(mlp_input, up_full, preferred_element_type=F32)
    activated = jnp.square(jax.nn.relu(up_proj * part(up_scale, 0))).astype(BF16)
    mlp_share = lax.psum_scatter(
        jnp.dot(activated, down_full, preferred_element_type=F32).astype(BF16),
        team, scatter_dimension=0, tiled=True,
    ).astype(F32)
    return (hidden_state.astype(F32) + unit_rows(mlp_share) * gains[1]).astype(BF16)[None]


def solution(mesh):
    in_specs = (
        P(("rep", "fs"), None, None),
        P("fs"), P("fs"), P("fs"), P("fs"),
        P("fs", "tp"), P("fs", "tp"),
        P("tp"), P("tp"),
        P(None, "tp"), P("tp", None), P("tp", None), P("tp"),
        P("tp", "fs"), P("fs"),
        P("fs", "tp"), P("tp"),
        P("tp", "fs"), P("fs"),
    )
    out_specs = P(("rep", "fs"), "tp", None)
    return jax.shard_map(
        on_device, mesh=mesh, in_specs=in_specs, out_specs=out_specs, check_vma=False
    )
```

```python
import functools

import jax
import jax.numpy as jnp
from jax import lax
from jax.experimental import pallas as pl
from jax.experimental.pallas import tpu as pltpu
from jax.sharding import PartitionSpec as P

BLOCK = 32
LANES = 128
EPSILON = 1e-06
DECAY_SCALE = 8.0
F32 = jnp.float32
BF16 = jnp.bfloat16


def unit_rows(values):
    return values * lax.rsqrt(jnp.mean(values * values, axis=-1, keepdims=True) + EPSILON)


def shifted(values, distance, fill):
    head = jnp.full((distance, values.shape[1]), fill, values.dtype)
    return jnp.concatenate([head, values[: values.shape[0] - distance]], axis=0)


def mixer_kernel(x_ref, gate_ref, taps_ref, recur_ref, input_ref, rate_ref, mixed_ref):
    length = x_ref.shape[0]
    x_branch = x_ref[...].astype(F32)
    taps = taps_ref.shape[0]
    total = taps_ref[taps - 1 : taps, :] * x_branch
    for tap in range(taps - 1):
        total += taps_ref[tap : tap + 1, :] * shifted(x_branch, taps - 1 - tap, 0.0)
    conv = total.astype(BF16)
    recur = jax.nn.sigmoid(jnp.dot(conv, recur_ref[...], preferred_element_type=F32))
    gate_in = jax.nn.sigmoid(jnp.dot(conv, input_ref[...], preferred_element_type=F32))
    log_decay = recur * rate_ref[0:1, :]
    decay = jnp.exp(log_decay)
    z = -2.0 * log_decay
    series = z * (1.0 - z * (1 / 2) * (1.0 - z * (1 / 3) * (1.0 - z * (1 / 4) * (1.0 - z * (1 / 5)))))
    power = jnp.where(z < 0.1, series, 1.0 - decay * decay)
    state = jnp.sqrt(power) * gate_in * conv.astype(F32)
    distance = 1
    while distance < length:
        state = state + decay * shifted(state, distance, 0.0)
        decay = decay * shifted(decay, distance, 1.0)
        distance *= 2
    mixed_ref[...] = (state * jax.nn.gelu(gate_ref[...].astype(F32))).astype(BF16)


def mixer(branches, taps, recur_dense, input_dense, rate, sequences):
    rows, width = branches.shape[0], branches.shape[1] // 2
    length = rows // sequences
    groups = width // LANES
    return pl.pallas_call(
        mixer_kernel,
        grid=(sequences, groups),
        in_specs=[
            pl.BlockSpec((length, LANES), lambda s, g: (s, g)),
            pl.BlockSpec((length, LANES), lambda s, g: (s, g + groups)),
            pl.BlockSpec((taps.shape[0], LANES), lambda s, g: (0, g)),
            pl.BlockSpec((LANES, LANES), lambda s, g: (g, 0)),
            pl.BlockSpec((LANES, LANES), lambda s, g: (g, 0)),
            pl.BlockSpec((1, LANES), lambda s, g: (0, g)),
        ],
        out_specs=pl.BlockSpec((length, LANES), lambda s, g: (s, g)),
        out_shape=jax.ShapeDtypeStruct((rows, width), BF16),
        cost_estimate=pl.CostEstimate(
            flops=rows * width * 100, bytes_accessed=rows * width * 6, transcendentals=rows * width * 4
        ),
        name="mixer",
    )(branches, branches, taps, recur_dense, input_dense, rate)


MESH_IDS = pl.DeviceIdType.MESH


def greet(peers):
    barrier = pltpu.get_barrier_semaphore()
    for peer in peers:
        pl.semaphore_signal(barrier, inc=1, device_id=peer, device_id_type=MESH_IDS)
    pl.semaphore_wait(barrier, len(peers))


def push(source, target, sent, landed, peer):
    return pltpu.make_async_remote_copy(
        src_ref=source, dst_ref=target, send_sem=sent, recv_sem=landed,
        device_id=peer, device_id_type=MESH_IDS,
    )


def others(axis, count):
    me = lax.axis_index(axis)
    return [lax.rem(me + step, count) for step in range(1, count)]


def row_block(ref, index, rows):
    return ref.at[pl.ds(pl.multiple_of(index * rows, rows), rows)]


def team_gather_kernel(reps, tps, x_ref, out_ref, own_sem, sent, landed):
    rep, core = lax.axis_index("rep"), lax.axis_index("tp")
    rows = x_ref.shape[0]
    rep_peers, tp_peers = others("rep", reps), others("tp", tps)
    greet([{"rep": peer} for peer in rep_peers] + [{"tp": peer} for peer in tp_peers])
    mine = row_block(out_ref, rep * tps + core, rows)
    flights = []
    for step, peer in enumerate(rep_peers):
        copy = push(x_ref, mine, sent.at[step + 1, 0], landed.at[step + 1, 0], {"rep": peer})
        copy.start()
        flights.append(copy)
    own = pltpu.make_async_copy(x_ref, mine, own_sem)
    own.start()
    local = []
    for slot, peer in enumerate(tp_peers):
        copy = push(x_ref, mine, sent.at[0, slot + 1], landed.at[0, slot + 1], {"tp": peer})
        copy.start()
        local.append(copy)
    for step in range(1, reps):
        flights[step - 1].wait_recv()
        source = lax.rem(rep + reps - step, reps)
        block = row_block(out_ref, source * tps + core, rows)
        for slot, peer in enumerate(tp_peers):
            copy = push(block, block, sent.at[step, slot + 1], landed.at[step, slot + 1], {"tp": peer})
            copy.start()
            local.append(copy)
    for copy in flights:
        copy.wait_send()
    for copy in local:
        copy.wait()
    own.wait()


def team_gather(values):
    reps, tps = lax.axis_size("rep"), lax.axis_size("tp")
    rows, width = values.shape
    return pl.pallas_call(
        functools.partial(team_gather_kernel, reps, tps),
        out_shape=jax.ShapeDtypeStruct((rows * reps * tps, width), values.dtype),
        in_specs=[pl.BlockSpec(memory_space=pltpu.VMEM)],
        out_specs=pl.BlockSpec(memory_space=pltpu.VMEM),
        scratch_shapes=[
            pltpu.SemaphoreType.DMA,
            pltpu.SemaphoreType.DMA((reps, tps)),
            pltpu.SemaphoreType.DMA((reps, tps)),
        ],
        compiler_params=pltpu.CompilerParams(collective_id=0, has_side_effects=True),
        cost_estimate=pl.CostEstimate(flops=0, bytes_accessed=80_000_000, transcendentals=0),
        name="team_gather",
    )(values)


def team_sum_kernel(reps, tps, part_ref, out_ref, got, stage, last, sent, landed, sent_far, landed_far):
    rep, core = lax.axis_index("rep"), lax.axis_index("tp")
    rows = out_ref.shape[0]
    step_rows = 16
    rep_peers, tp_peers = others("rep", reps), others("tp", tps)
    greet([{"rep": peer} for peer in rep_peers] + [{"tp": peer} for peer in tp_peers])
    near = []
    for slot, peer in enumerate(tp_peers):
        for group in range(reps):
            copy = push(
                row_block(part_ref, group * tps + peer, rows), got.at[slot, group],
                sent.at[slot, group], landed.at[slot, group], {"tp": peer},
            )
            copy.start()
            near.append(copy)
    for copy in near:
        copy.wait()

    def total(group, start):
        base = pl.multiple_of((group * tps + core) * rows + start, step_rows)
        value = part_ref[pl.ds(base, step_rows)].astype(F32)
        for slot in range(tps - 1):
            value += got[slot, group, pl.ds(start, step_rows)].astype(F32)
        return value

    far = []
    for step, peer in enumerate(rep_peers):

        def fill(index, carry):
            start = pl.multiple_of(index * step_rows, step_rows)
            stage[step, pl.ds(start, step_rows)] = total(peer, start).astype(BF16)
            return carry

        lax.fori_loop(0, rows // step_rows, fill, 0)
        copy = push(stage.at[step], last.at[step], sent_far.at[step], landed_far.at[step], {"rep": peer})
        copy.start()
        far.append(copy)
    for copy in far:
        copy.wait()

    def finish(index, carry):
        start = pl.multiple_of(index * step_rows, step_rows)
        value = total(rep, start)
        for step in range(reps - 1):
            value += last[step, pl.ds(start, step_rows)].astype(F32)
        out_ref[pl.ds(start, step_rows)] = value
        return carry

    lax.fori_loop(0, rows // step_rows, finish, 0)


def team_sum(parts):
    reps, tps = lax.axis_size("rep"), lax.axis_size("tp")
    rows, width = parts.shape[0] // (reps * tps), parts.shape[1]
    return pl.pallas_call(
        functools.partial(team_sum_kernel, reps, tps),
        out_shape=jax.ShapeDtypeStruct((rows, width), F32),
        in_specs=[pl.BlockSpec(memory_space=pltpu.VMEM)],
        out_specs=pl.BlockSpec(memory_space=pltpu.VMEM),
        scratch_shapes=[
            pltpu.VMEM((tps - 1, reps, rows, width), BF16),
            pltpu.VMEM((reps - 1, rows, width), BF16),
            pltpu.VMEM((reps - 1, rows, width), BF16),
            pltpu.SemaphoreType.DMA((tps - 1, reps)),
            pltpu.SemaphoreType.DMA((tps - 1, reps)),
            pltpu.SemaphoreType.DMA((reps - 1,)),
            pltpu.SemaphoreType.DMA((reps - 1,)),
        ],
        compiler_params=pltpu.CompilerParams(collective_id=1, has_side_effects=True),
        cost_estimate=pl.CostEstimate(flops=0, bytes_accessed=80_000_000, transcendentals=0),
        name="team_sum",
    )(parts)


def shard_gather_kernel(shards, x_ref, out_ref, own_sem, sent, landed, sent_pass, landed_pass):
    me = lax.axis_index("fs")
    rows = x_ref.shape[0]
    pairs = shards // 2
    pair, parity = me // 2, lax.rem(me, 2)
    partner = {"fs": pair * 2 + 1 - parity}
    peers = [{"fs": lax.rem(pair + step, pairs) * 2 + parity} for step in range(1, pairs)]
    greet([partner] + peers)
    mine = row_block(out_ref, me, rows)
    passed = [push(x_ref, mine, sent_pass.at[0], landed_pass.at[0], partner)]
    passed[0].start()
    direct = []
    for step, peer in enumerate(peers):
        copy = push(x_ref, mine, sent.at[step], landed.at[step], peer)
        copy.start()
        direct.append(copy)
    own = pltpu.make_async_copy(x_ref, mine, own_sem)
    own.start()
    for step in range(1, pairs):
        direct[step - 1].wait_recv()
        block = row_block(out_ref, lax.rem(pair + pairs - step, pairs) * 2 + parity, rows)
        copy = push(block, block, sent_pass.at[step], landed_pass.at[step], partner)
        copy.start()
        passed.append(copy)
    for copy in direct:
        copy.wait_send()
    for copy in passed:
        copy.wait()
    own.wait()


def shard_gather(values, collective_id):
    shards = lax.axis_size("fs")
    rows, width = values.shape
    return pl.pallas_call(
        functools.partial(shard_gather_kernel, shards),
        out_shape=jax.ShapeDtypeStruct((rows * shards, width), values.dtype),
        in_specs=[pl.BlockSpec(memory_space=pltpu.VMEM)],
        out_specs=pl.BlockSpec(memory_space=pltpu.VMEM),
        scratch_shapes=[
            pltpu.SemaphoreType.DMA,
            pltpu.SemaphoreType.DMA((shards // 2,)),
            pltpu.SemaphoreType.DMA((shards // 2,)),
            pltpu.SemaphoreType.DMA((shards // 2,)),
            pltpu.SemaphoreType.DMA((shards // 2,)),
        ],
        compiler_params=pltpu.CompilerParams(collective_id=collective_id, has_side_effects=True),
        cost_estimate=pl.CostEstimate(flops=0, bytes_accessed=200_000_000, transcendentals=0),
        name="shard_gather",
    )(values)


def on_device(
    tokens, gain_mix_pre, gain_mix_post, gain_mlp_pre, gain_mlp_post,
    x_weight, gate_weight, x_scale, gate_scale, conv_weight, recur_map, input_map,
    decay_param, out_weight, out_scale, up_weight, up_scale, down_weight, down_scale,
):
    reps = lax.axis_size("rep")
    rep = lax.axis_index("rep")

    def part(values, axis):
        size = values.shape[axis] // reps
        return lax.dynamic_slice_in_dim(values, rep * size, size, axis)

    length = tokens.shape[1]
    share_rows = length // lax.axis_size("tp")
    offset_row = lax.axis_index("tp") * share_rows
    resid_share = lax.dynamic_slice_in_dim(tokens[0], offset_row, share_rows, 0).astype(F32)
    normed_share = unit_rows(resid_share).astype(BF16)

    pre = gain_mix_pre[:, None]
    branch_rows = jnp.concatenate(
        [(part(x_weight, 1) * pre).astype(BF16), (part(gate_weight, 1) * pre).astype(BF16)], axis=1
    )
    branch_rows, out_weight = lax.optimization_barrier((branch_rows, out_weight))
    branch_full = lax.all_gather(branch_rows, "fs", axis=0, tiled=True)
    post = jnp.stack([gain_mix_post, gain_mlp_post])
    post_high = post.astype(BF16)
    post_low = (post - post_high.astype(F32)).astype(BF16)
    pad_rows = jnp.zeros((12, post.shape[1]), BF16)
    out_cols = jnp.concatenate(
        [(part(out_weight, 0) * out_scale).astype(BF16), post_high, post_low, pad_rows], axis=0
    )
    out_cols, down_weight = lax.optimization_barrier((out_cols, down_weight))
    out_all = lax.all_gather(out_cols, "fs", axis=1, tiled=True)
    down_full = lax.all_gather((part(down_weight, 0) * down_scale).astype(BF16), "fs", axis=1, tiled=True)
    up_rows = (part(up_weight, 1) * gain_mlp_pre[:, None]).astype(BF16)
    normed = team_gather(normed_share)
    normed, up_rows = lax.optimization_barrier((normed, up_rows))
    up_full = shard_gather(up_rows, 2)
    normed, up_full = lax.optimization_barrier((normed, up_full))

    scales = jnp.concatenate([part(x_scale, 0), part(gate_scale, 0)])
    branches = (jnp.dot(normed, branch_full, preferred_element_type=F32) * scales).astype(BF16)
    width = branches.shape[1] // 2

    def dense(block_map):
        rows = lax.broadcasted_iota(jnp.int32, (width, LANES), 0)
        columns = lax.broadcasted_iota(jnp.int32, (width, LANES), 1)
        spread = jnp.tile(part(block_map, 0), (1, LANES // BLOCK))
        return jnp.where(rows % LANES // BLOCK == columns // BLOCK, spread, 0).astype(BF16)

    rate = -DECAY_SCALE * jax.nn.softplus(-part(decay_param, 0))
    mixed = mixer(
        branches, part(conv_weight, 1), dense(recur_map), dense(input_map), rate[None], reps
    )
    out_full = out_all[:width]
    gains = out_all[width : width + 2].astype(F32) + out_all[width + 2 : width + 4].astype(F32)
    mix_share = team_sum(jnp.dot(mixed, out_full, preferred_element_type=F32).astype(BF16))
    hidden_state = (resid_share + unit_rows(mix_share) * gains[0]).astype(BF16)
    mlp_input = team_gather(unit_rows(hidden_state.astype(F32)).astype(BF16))
    up_proj = jnp.dot(mlp_input, up_full, preferred_element_type=F32)
    activated = jnp.square(jax.nn.relu(up_proj * part(up_scale, 0))).astype(BF16)
    mlp_share = team_sum(jnp.dot(activated, down_full, preferred_element_type=F32).astype(BF16))
    return (hidden_state.astype(F32) + unit_rows(mlp_share) * gains[1]).astype(BF16)[None]


def solution(mesh):
    in_specs = (
        P(("rep", "fs"), None, None),
        P("fs"), P("fs"), P("fs"), P("fs"),
        P("fs", "tp"), P("fs", "tp"),
        P("tp"), P("tp"),
        P(None, "tp"), P("tp", None), P("tp", None), P("tp"),
        P("tp", "fs"), P("fs"),
        P("fs", "tp"), P("tp"),
        P("tp", "fs"), P("fs"),
    )
    out_specs = P(("rep", "fs"), "tp", None)
    return jax.shard_map(
        on_device, mesh=mesh, in_specs=in_specs, out_specs=out_specs, check_vma=False
    )
```
